32 devices in a mesh: ep: 8 (over z, core), tp: 4 (over y, x).
Axes of the slice: x: 2, y: 2, z: 4, core: 2. Of those that a mesh axis runs over, the one named last changes fastest.
Arguments:
- tokens: bfloat16 [1024, 2048], P('ep'), may hold values from -6 to 6
- cotangent: bfloat16 [1024, 2048], P('ep'), may hold values from -6 to 6
- expert_ids: int32 [1024, 2], P('ep'), may hold values from 0 to 7, all different within a row; in each aligned block of 128 rows (0 to 127, 128 to 255, ...) at most 64 rows name the same one
- route_weight: bfloat16 [1024, 2], P('ep'), may hold values from 0.19921875 to 1
- gate_weight: bfloat16 [8, 1024, 2048], P('ep', 'tp'), may hold values from -0.125 to 0.125
- up_weight: bfloat16 [8, 1024, 2048], P('ep', 'tp'), may hold values from -0.125 to 0.125
- down_weight: bfloat16 [8, 1024, 2048], P('ep', 'tp'), may hold values from -0.1875 to 0.1875
Outputs:
- tokens_grad: bfloat16 [1024, 2048], P('ep', 'tp')
- route_weight_grad: float32 [1024, 2], P('ep')
- gate_weight_grad: float32 [8, 1024, 2048], P('ep', 'tp')
- up_weight_grad: float32 [8, 1024, 2048], P('ep', 'tp')
- down_weight_grad: float32 [8, 1024, 2048], P('ep', 'tp')
The draws below stay inside these ranges and needn't reach their ends.
Inputs may be any that keep to these rules, and one draw needn't show every extreme that they name: `expert_ids`: within each aligned block of 128 rows every expert is named at most 64 times; the two experts of a row differ.
All inputs are finite; a program needn't handle non-finite values.
Results may differ from the reference program's by a relative error of at most 0.0058.
Values may be sent and summed in bfloat16 or wider, within the bound.
A program may use at most 64 MiB of HBM per device.

```python
import math
import jax
import jax.numpy as jnp
import numpy as np
from jax import lax

D = 2048
FE = 1024
TOP = 2
TOK_DEV = 128
EXPERTS = 8
TOKENS = 1024
CAP = 64
N_EP = 8


def block_scale(rng, shape, split, smallest, high):
    loudness, own = 1.0, jax.random.fold_in(rng, 6)
    for axis_at, parts in split:
        draws = jnp.exp(jax.random.uniform(jax.random.fold_in(own, axis_at), (parts,), jnp.float32, smallest / len(split), high / len(split)))
        loudness = loudness * jnp.repeat(draws, shape[axis_at] // parts).reshape([-1 if axis == axis_at else 1 for axis in range(len(shape))])
    return loudness


def assign_block(own_key, own, number, rows, count, top, most, slope):
    sequence = jax.random.permutation(own_key, count)
    crowded, common = load_shares(count, rows * top, most, slope, True), load_shares(count, rows * top, most, slope, False)
    places = jnp.arange(count)

    def named(tallies, turn):
        used = int((tallies > 0).sum())
        fixed = max(1, used // 4)
        shifted = fixed + (places - fixed + turn * (used - fixed)) % max(1, count - fixed)
        return jnp.zeros((count,), jnp.int32).at[sequence[jnp.where(places < fixed, places, shifted)]].set(jnp.asarray(tallies, jnp.int32))

    tallies = jnp.where(number % 4 == 0, named(crowded, number // 4), named(common, number - number // 4 - 1))
    mixed = jax.random.permutation(jax.random.fold_in(own, 3), count)
    source_of, taker = mixed[0:count // 2 * 2:2], mixed[1:count // 2 * 2:2]
    slack = jnp.minimum(tallies[source_of] - 1, most - tallies[taker]) // 2
    slack = jnp.where((source_of == sequence[0]) | (taker == sequence[0]) | (tallies[taker] == 0), 0, jnp.maximum(slack, 0))
    shifted = jax.random.randint(jax.random.fold_in(own, 4), (count // 2,), 0, 1 << 20) % (slack + 1)
    tallies = tallies.at[source_of].add(-shifted).at[taker].add(shifted)
    items = jnp.searchsorted(jnp.cumsum(tallies), jnp.arange(rows * top), side="right").astype(jnp.int32)
    listing = items.reshape(top, rows).T
    listing = listing[jax.random.permutation(jax.random.fold_in(own, 1), rows)]
    turn = jax.random.randint(jax.random.fold_in(own, 2), (rows, 1), 0, top)
    return jnp.take_along_axis(listing, (jnp.arange(top)[None, :] + turn) % top, axis=1)


def load_shares(amount, total, most, slope, full):
    portions = [(1 << 20) // math.isqrt(rank ** slope) + 1 for rank in range(1, amount + 1)]
    largest = most if full else min(most, max(-(-total // amount), total * portions[0] // sum(portions)))
    least = 1 if total - largest >= amount - 1 else 0
    given, spare = [largest] + [least] * (amount - 1), total - largest - least * (amount - 1)
    while spare > 0:
        free = [i for i in range(1, amount) if given[i] < largest] or [i for i in range(1, amount) if given[i] < most]
        whole, left = sum([portions[i] for i in free]), spare
        for i in free:
            extra = min(most - given[i], max(1, left * portions[i] // whole), spare)
            given[i] = given[i] + extra
            spare = spare - extra
    return np.array(given)


def gaussian(stream_key, shape, spread, reach, cuts=(), kind=jnp.bfloat16):
    entries = spread * jax.random.normal(stream_key, shape, jnp.float32)
    if cuts:
        entries = entries * block_scale(stream_key, shape, cuts, -0.22, 0.18)
    return jnp.clip(entries, -reach, reach).astype(kind)


def setup_inputs(seed: int = 0) -> dict:
    streams_of = jax.random.split(jax.random.key(seed), 8)
    tokens = gaussian(streams_of[0], (TOKENS, D), 1.0, 6.0, ((0, 8),))
    cotangent = gaussian(streams_of[1], (TOKENS, D), 1.0, 6.0, ((0, 8),))
    expert_ids_keys = jax.random.split(jax.random.fold_in(streams_of[2], 1), TOKENS // TOK_DEV)
    expert_ids_turns = jax.random.permutation(jax.random.fold_in(streams_of[2], 3), TOKENS // TOK_DEV)
    expert_ids = jax.vmap(lambda own, number: assign_block(jax.random.fold_in(streams_of[2], 2), own, number, TOK_DEV, EXPERTS, TOP, CAP, 2))(expert_ids_keys, expert_ids_turns).reshape((TOKENS, TOP))
    route_weight = jnp.clip(0.19921875 + 0.80078125 * jax.random.uniform(streams_of[3], (TOKENS, TOP), jnp.float32) ** block_scale(streams_of[3], (TOKENS, TOP), ((0, 8),), -0.2, 0.2), 0.19921875, 1.0).astype(jnp.bfloat16)
    gate_weight = gaussian(streams_of[4], (EXPERTS, FE, D), D ** -0.5, 0.125, ((0, 8), (1, 4)))
    up_weight = gaussian(streams_of[5], (EXPERTS, FE, D), D ** -0.5, 0.125, ((0, 8), (1, 4)))
    down_weight = gaussian(streams_of[6], (EXPERTS, FE, D), FE ** -0.5, 0.1875, ((0, 8), (1, 4)))
    return {"tokens": tokens, "cotangent": cotangent, "expert_ids": expert_ids, "route_weight": route_weight, "gate_weight": gate_weight, "up_weight": up_weight, "down_weight": down_weight}


def reference(tokens, cotangent, expert_ids, route_weight, gate_weight, up_weight, down_weight):
    routed = TOKENS * TOP
    buffer_rows = N_EP * CAP
    flat_ids = expert_ids.reshape(-1)
    flat_weight = route_weight.reshape(-1)

    def one_expert(expert):
        picked = jnp.nonzero(flat_ids == expert, size=buffer_rows, fill_value=routed)[0].astype(jnp.int32)
        usable = picked < routed
        safe_pair = jnp.minimum(picked, routed - 1)
        token_of = safe_pair // TOP
        routed_rows = tokens[token_of]
        routed_cotangent = cotangent[token_of]
        weight = jnp.where(usable, flat_weight[safe_pair].astype(jnp.float32), jnp.float32(0.0))[:, None]
        gate_w = lax.dynamic_index_in_dim(gate_weight, expert, 0, keepdims=False)
        up_w = lax.dynamic_index_in_dim(up_weight, expert, 0, keepdims=False)
        down_w = lax.dynamic_index_in_dim(down_weight, expert, 0, keepdims=False)
        pre_gate = jnp.dot(routed_rows, gate_w.T, preferred_element_type=jnp.float32)
        pre_up = jnp.dot(routed_rows, up_w.T, preferred_element_type=jnp.float32)
        sigma = jax.nn.sigmoid(pre_gate)
        silu_gate = pre_gate * sigma
        hidden = silu_gate * pre_up
        back_hidden = jnp.dot(routed_cotangent, down_w.T, preferred_element_type=jnp.float32)
        products = jnp.sum(hidden * back_hidden, axis=1)
        scaled = weight * back_hidden
        grad_gate = (scaled * pre_up * sigma * (1.0 + pre_gate * (1.0 - sigma))).astype(jnp.bfloat16)
        grad_up = (scaled * silu_gate).astype(jnp.bfloat16)
        weighted = (weight * hidden).astype(jnp.bfloat16)
        down_grad = jnp.dot(weighted.T, routed_cotangent, preferred_element_type=jnp.float32)
        gate_grad = jnp.dot(grad_gate.T, routed_rows, preferred_element_type=jnp.float32)
        up_grad = jnp.dot(grad_up.T, routed_rows, preferred_element_type=jnp.float32)
        pair_grad = (jnp.dot(grad_gate, gate_w, preferred_element_type=jnp.float32)
                     + jnp.dot(grad_up, up_w, preferred_element_type=jnp.float32)).astype(jnp.bfloat16)
        return gate_grad, up_grad, down_grad, picked, pair_grad, products

    gate_grad, up_grad, down_grad, picked, pair_grad, products = lax.map(
        one_expert, jnp.arange(EXPERTS, dtype=jnp.int32))
    slot_flat = picked.reshape(-1)
    token_sum = jnp.zeros((routed, D), jnp.float32).at[slot_flat].set(
        pair_grad.reshape(-1, D).astype(jnp.float32), mode="drop")
    tokens_grad = jnp.sum(token_sum.reshape(TOKENS, TOP, D), axis=1).astype(jnp.bfloat16)
    route_grad = jnp.zeros((routed,), jnp.float32).at[slot_flat].set(products.reshape(-1), mode="drop")
    return tokens_grad, route_grad.reshape(TOKENS, TOP), gate_grad, up_grad, down_grad
```

```python
import functools

import jax
import jax.numpy as jnp
from jax import lax
from jax.experimental import pallas as pl
from jax.experimental.pallas import tpu as pltpu
from jax.sharding import PartitionSpec as P

MESH = pl.DeviceIdType.MESH
F32 = jnp.float32
BF16 = jnp.bfloat16


def slices_for(j, tp, bits, count):
    base = j
    for bit in bits:
        base = base - ((j // bit) % 2) * bit
    out = []
    for k in range(count):
        out.append(base + sum(bit for n, bit in enumerate(bits) if (k >> n) & 1))
    return out


def kernel(
    ep, tp, tokens, cotangent, pair_w, gate_w, up_w, down_w,
    dx_out, route_out, gate_out, up_out, down_out,
    rows, weights, wg, part, core_in, tp_in, z_in, grads, totals, r_send, r_in, r_tp,
    load_sem, wz_send, wz_recv, z_send, z_recv, t_send, t_recv, c_send, c_recv,
    pc_send, pc_recv, pt_send, pt_recv, pz_send, pz_recv, rs_send, rs_recv, rt_send, rt_recv, out_sem,
):
    e, j = lax.axis_index("ep"), lax.axis_index("tp")
    levels = ep // 2
    lvl, core = e // 2, e % 2
    t_rows, width = tokens.shape
    span = width // tp
    half = t_rows // 2
    f_rows = gate_w.shape[0]
    nb = tp.bit_length() - 1
    slots = part.shape[0]
    mate = 2 * lvl + 1 - core

    def order(i):
        near = jnp.minimum(lvl, levels - 1 - lvl)
        d = (i + 1) // 2
        close = jnp.where(i % 2 == 1, lvl - d, lvl + d)
        far = jnp.where(lvl == near, lvl + (i - near), lvl - (i - near))
        return jnp.where(i <= 2 * near, close, far)

    def row0(l, c):
        return pl.multiple_of((2 * l + c) * t_rows, t_rows)

    def col(s):
        return pl.ds(pl.multiple_of(s * span, span), span)

    def flip(bit):
        return j + bit * (1 - 2 * ((j // bit) % 2))

    def remote(src, dst, ssem, rsem, de, dt):
        return pltpu.make_async_remote_copy(
            src_ref=src, dst_ref=dst, send_sem=ssem, recv_sem=rsem,
            device_id=(de, dt), device_id_type=MESH)

    own = pl.ds(row0(lvl, core), t_rows)
    loads = [
        pltpu.make_async_copy(tokens, rows.at[0, own], load_sem.at[0]),
        pltpu.make_async_copy(cotangent, rows.at[1, own], load_sem.at[1]),
        pltpu.make_async_copy(gate_w, weights.at[0], load_sem.at[2]),
        pltpu.make_async_copy(up_w, weights.at[1], load_sem.at[3]),
        pltpu.make_async_copy(down_w, weights.at[2], load_sem.at[4]),
    ]
    for copy in loads:
        copy.start()
    barrier = pltpu.get_barrier_semaphore()

    def greet(n, _):
        pl.semaphore_signal(barrier, inc=1, device_id=(lax.rem(e + n, ep), j), device_id_type=MESH)
        return 0

    def greet_tp(n, _):
        pl.semaphore_signal(barrier, inc=1, device_id=(e, lax.rem(j + n, tp)), device_id_type=MESH)
        return 0

    lax.fori_loop(1, ep, greet, 0)
    lax.fori_loop(1, tp, greet_tp, 0)
    pl.semaphore_wait(barrier, ep + tp - 2)

    def w_copy(d):
        return remote(pair_w.at[d], wg.at[e], wz_send.at[d], wz_recv.at[e], d, j)

    def w_wait(src):
        return remote(pair_w.at[src], wg.at[src], wz_send.at[src], wz_recv.at[src], src, j)

    def z_copy(a, l, side):
        ref = rows.at[a, pl.ds(row0(l, core), t_rows), col(j)]
        de = lax.rem(e + (2 if side else ep - 2), ep)
        return remote(ref, ref, z_send.at[a, side, l], z_recv.at[a, l], de, j)

    def gather_step(a, l, s, receive):
        copies = []
        for h in range(2):
            order_bits = [1 << b for b in (range(nb) if h == 0 else range(nb - 1, -1, -1))]
            peer = flip(order_bits[s])
            ids = slices_for(peer if receive else j, tp, order_bits[:s], 1 << s)
            for k, sid in enumerate(ids):
                ref = rows.at[a, pl.ds(row0(l, core) + h * half, half), col(sid)]
                copies.append(remote(
                    ref, ref, t_send.at[a, l, h, (1 << s) - 1 + k], t_recv.at[a, l, h, sid], e, peer))
        return copies

    def core_copy(a, l, c):
        ref = rows.at[a, pl.ds(row0(l, c), t_rows)]
        return remote(ref, ref, c_send.at[a, l], c_recv.at[a, l], mate, j)

    def pc_copy(l, i):
        return remote(part.at[i % slots, 1 - core], core_in.at[l], pc_send.at[l], pc_recv.at[l], mate, j)

    def scatter_step(l, i, s, receive):
        copies = []
        base = sum(tp >> (n + 1) for n in range(s))
        count = tp >> (s + 1)
        for h in range(2):
            order_bits = [1 << b for b in (range(nb) if h == 0 else range(nb - 1, -1, -1))]
            peer = flip(order_bits[s])
            ids = slices_for(j if receive else peer, tp, order_bits[s + 1:], count)
            for k, sid in enumerate(ids):
                src = part.at[i % slots, core, pl.ds(h * half, half), col(sid)]
                dst = tp_in.at[l, h, base + k]
                copies.append((remote(src, dst, pt_send.at[l, h, base + k], pt_recv.at[l, h, base + k], e, peer),
                               src, dst))
        return copies

    def pz_copy(l, i):
        return remote(part.at[i % slots, core, :, col(j)], z_in.at[lvl], pz_send.at[l], pz_recv.at[lvl],
                      2 * l + core, j)

    def pz_wait(src):
        return remote(part.at[0, core, :, col(j)], z_in.at[src], pz_send.at[src], pz_recv.at[src],
                      2 * src + core, j)

    for n in range(2):
        loads[n].wait()
        @pl.when(lvl + 1 < levels)
        def _():
            z_copy(n, lvl, 1).start()
        @pl.when(lvl > 0)
        def _():
            z_copy(n, lvl, 0).start()
        core_copy(n, lvl, core).start()

    def w_start(n, _):
        w_copy(lax.rem(e + n, ep)).start()
        return 0

    lax.fori_loop(1, ep, w_start, 0)
    wg[e] = pair_w[e]
    for n in range(2, 5):
        loads[n].wait()

    def arrive(i):
        l = order(i)
        for a in range(2):
            z_copy(a, l, 0).wait_recv()
            @pl.when(jnp.logical_and(l < lvl, lvl + 1 < levels))
            def _():
                z_copy(a, l, 1).start()
            @pl.when(jnp.logical_and(l > lvl, lvl > 0))
            def _():
                z_copy(a, l, 0).start()
            for copy in gather_step(a, l, 0, False):
                copy.start()

    def spread(i, s):
        l = order(i)
        for a in range(2):
            for copy in gather_step(a, l, s - 1, True):
                copy.wait_recv()
            if s < nb:
                for copy in gather_step(a, l, s, False):
                    copy.start()
            else:
                core_copy(a, l, core).start()

    def compute(i):
        l = order(i)
        for a in range(2):
            core_copy(a, l, 1 - core).wait_recv()
        @pl.when(l != lvl)
        def _():
            w_wait(2 * l).wait_recv()
            w_wait(2 * l + 1).wait_recv()
        @pl.when(l == lvl)
        def _():
            w_wait(mate).wait_recv()
        sel = pl.ds(row0(l, 0), 2 * t_rows)
        nt = (((1,), (1,)), ((), ()))
        x = rows[0, sel, :]
        pre_gate = lax.dot_general(weights[0], x, nt, preferred_element_type=F32)
        pre_up = lax.dot_general(weights[1], x, nt, preferred_element_type=F32)
        back = lax.dot_general(weights[2], rows[1, sel, :], nt, preferred_element_type=F32)
        p = jnp.concatenate([wg[2 * l], wg[2 * l + 1]], axis=1)
        sigma = jax.nn.sigmoid(pre_gate)
        silu = pre_gate * sigma
        hidden = silu * pre_up
        prod = jnp.sum(hidden * back, axis=0, keepdims=True)
        r_send[2 * l] = prod[:, :t_rows]
        r_send[2 * l + 1] = prod[:, t_rows:]
        scaled = p * back
        gg = (scaled * pre_up * sigma * (1.0 + pre_gate * (1.0 - sigma))).astype(BF16)
        gu = (scaled * silu).astype(BF16)
        grads[0, :, sel] = gg
        grads[1, :, sel] = gu
        grads[2, :, sel] = (p * hidden).astype(BF16)
        ggt, gut = gg.T, gu.T
        tile = min(width, 512)

        def column(n, _):
            cs = pl.ds(pl.multiple_of(n * tile, tile), tile)
            d = (jnp.dot(ggt, weights[0, :, cs], preferred_element_type=F32)
                 + jnp.dot(gut, weights[1, :, cs], preferred_element_type=F32)).astype(BF16)
            part[i % slots, 0, :, cs] = d[:t_rows]
            part[i % slots, 1, :, cs] = d[t_rows:]
            return 0

        lax.fori_loop(0, width // tile, column, 0)
        pc_copy(l, i).start()

        def send_r(d):
            remote(r_send.at[d], r_in.at[e], rs_send.at[d], rs_recv.at[e], d, j).start()
        for c in range(2):
            @pl.when(2 * l + c != e)
            def _():
                send_r(2 * l + c)
            @pl.when(2 * l + c == e)
            def _():
                r_in[2 * l + c] = r_send[2 * l + c]

    def merge_core(i):
        l = order(i)
        pc_copy(l, i).wait()
        part[i % slots, core] = (part[i % slots, core].astype(F32) + core_in[l].astype(F32)).astype(BF16)
        for copy, _, _ in scatter_step(l, i, 0, False):
            copy.start()

    def merge_tp(i, s):
        l = order(i)
        for (copy, _, _), (_, mine, got) in zip(scatter_step(l, i, s, False), scatter_step(l, i, s, True)):
            copy.wait()
            mine[...] = (mine[...].astype(F32) + got[...].astype(F32)).astype(BF16)
        if s + 1 < nb:
            for copy, _, _ in scatter_step(l, i, s + 1, False):
                copy.start()
        else:
            @pl.when(l != lvl)
            def _():
                pz_copy(l, i).start()
            @pl.when(l == lvl)
            def _():
                z_in[lvl] = part[i % slots, core, :, col(j)]

    def drain(i):
        l = order(i)
        @pl.when(l != lvl)
        def _():
            pz_copy(l, i).wait_send()

    outs = (gate_out, up_out, down_out)

    def out_copy(k):
        return pltpu.make_async_copy(totals.at[k], outs[k], out_sem.at[k])

    def weight_grad(k):
        tile = min(width, 512)

        def column(n, _):
            cs = pl.ds(pl.multiple_of(n * tile, tile), tile)
            totals[k, :, cs] = jnp.dot(grads[k], rows[k // 2, :, cs], preferred_element_type=F32)
            return 0

        lax.fori_loop(0, width // tile, column, 0)
        out_copy(k).start()

    compute(0)
    d_comp = nb + 2
    last = levels - 1 + d_comp

    def tick(t, _):
        def stage(f, i, low):
            @pl.when(jnp.logical_and(i >= low, i < levels))
            def _():
                f(i)
        def back(late):
            return jnp.where(t == 1 + late, 0, jnp.where(t > d_comp + late, t - d_comp - late, -1))

        stage(drain, back(nb + 1), 0)
        for s in range(nb - 1, -1, -1):
            stage(functools.partial(merge_tp, s=s), back(1 + s), 0)
        stage(arrive, t, 1)
        for s in range(1, nb + 1):
            stage(functools.partial(spread, s=s), t - s, 1)
        stage(compute, t - d_comp + 1, 1)
        stage(merge_core, back(0), 0)
        for k in range(3):
            @pl.when(t == last + k)
            def _():
                weight_grad(k)
        return 0

    lax.fori_loop(1, levels + d_comp + nb + 1, tick, 0)

    def r_wait(n, _):
        src = lax.rem(e + n, ep)
        remote(r_send.at[src], r_in.at[src], rs_send.at[src], rs_recv.at[src], src, j).wait()
        return 0

    lax.fori_loop(1, ep, r_wait, 0)

    def rt_copy(n):
        dt = lax.rem(j + n, tp)
        return remote(r_in, r_tp.at[j], rt_send.at[dt], rt_recv.at[j], e, dt)

    def rt_wait(n, _):
        src = lax.rem(j + n, tp)
        remote(r_in, r_tp.at[src], rt_send.at[src], rt_recv.at[src], e, src).wait()
        return 0

    def rt_start(n, _):
        rt_copy(n).start()
        return 0

    lax.fori_loop(1, tp, rt_start, 0)
    r_tp[j] = r_in[...]

    def pz_drain(src, _):
        @pl.when(src != lvl)
        def _():
            pz_wait(src).wait_recv()
        return 0

    lax.fori_loop(0, levels, pz_drain, 0)
    dx_out[...] = jnp.sum(z_in[...].astype(F32), axis=0).astype(BF16)
    lax.fori_loop(1, tp, rt_wait, 0)
    route_out[...] = jnp.sum(r_tp[...], axis=0)

    for a in range(2):
        @pl.when(lvl + 1 < levels)
        def _():
            z_copy(a, lvl, 1).wait_send()
        @pl.when(lvl > 0)
        def _():
            z_copy(a, lvl, 0).wait_send()

    def finish(l, _):
        for a in range(2):
            core_copy(a, l, core).wait_send()
            @pl.when(jnp.logical_and(l < lvl, lvl + 1 < levels))
            def _():
                z_copy(a, l, 1).wait_send()
            @pl.when(jnp.logical_and(l > lvl, lvl > 0))
            def _():
                z_copy(a, l, 0).wait_send()
            @pl.when(l != lvl)
            def _():
                for s in range(nb):
                    for copy in gather_step(a, l, s, False):
                        copy.wait_send()
        return 0

    lax.fori_loop(0, levels, finish, 0)

    def w_done(n, _):
        w_copy(lax.rem(e + n, ep)).wait_send()
        return 0

    lax.fori_loop(1, ep, w_done, 0)
    for k in range(3):
        out_copy(k).wait()


def per_device(tokens, cotangent, expert_ids, route_weight, gate_weight, up_weight, down_weight):
    ep, tp = lax.axis_size("ep"), lax.axis_size("tp")
    t_rows, width = tokens.shape
    _, f_rows, _ = gate_weight.shape
    levels = ep // 2
    span = width // tp
    slots = min(levels, 8)
    named = expert_ids.T[:, None, :] == jnp.arange(ep, dtype=jnp.int32)[None, :, None]
    pair_w = jnp.sum(jnp.where(named, route_weight.T[:, None, :].astype(F32), 0.0), axis=0)
    pair_w = pair_w.reshape(ep, 1, t_rows)
    any_, vmem = pl.BlockSpec(memory_space=pl.ANY), pl.BlockSpec(memory_space=pltpu.VMEM)
    dma = pltpu.SemaphoreType.DMA
    big = jax.ShapeDtypeStruct((f_rows, width), F32)
    scratch = [
        pltpu.VMEM((2, ep * t_rows, width), BF16),
        pltpu.VMEM((3, f_rows, width), BF16),
        pltpu.VMEM((ep, 1, t_rows), F32),
        pltpu.VMEM((slots, 2, t_rows, width), BF16),
        pltpu.VMEM((levels, t_rows, width), BF16),
        pltpu.VMEM((levels, 2, tp - 1, t_rows // 2, span), BF16),
        pltpu.VMEM((levels, t_rows, span), BF16),
        pltpu.VMEM((3, f_rows, ep * t_rows), BF16),
        pltpu.VMEM((3, f_rows, width), F32),
        pltpu.VMEM((ep, 1, t_rows), F32),
        pltpu.VMEM((ep, 1, t_rows), F32),
        pltpu.VMEM((tp, ep, 1, t_rows), F32),
        dma((5,)), dma((ep,)), dma((ep,)), dma((2, 2, levels)), dma((2, levels)),
        dma((2, levels, 2, tp - 1)), dma((2, levels, 2, tp)), dma((2, levels)), dma((2, levels)),
        dma((levels,)), dma((levels,)), dma((levels, 2, tp - 1)), dma((levels, 2, tp - 1)),
        dma((levels,)), dma((levels,)), dma((ep,)), dma((ep,)), dma((tp,)), dma((tp,)), dma((3,)),
    ]
    dx, route, gate_grad, up_grad, down_grad = pl.pallas_call(
        functools.partial(kernel, ep, tp),
        out_shape=(
            jax.ShapeDtypeStruct((t_rows, span), BF16),
            jax.ShapeDtypeStruct((ep, 1, t_rows), F32), big, big, big),
        in_specs=[any_, any_, vmem, any_, any_, any_],
        out_specs=(vmem, vmem, any_, any_, any_),
        scratch_shapes=scratch,
        compiler_params=pltpu.CompilerParams(
            collective_id=0, has_side_effects=True, vmem_limit_bytes=66_000_000),
    )(tokens, cotangent, pair_w, gate_weight[0], up_weight[0], down_weight[0])
    route_grad = jnp.sum(jnp.where(named, route[None, :, 0, :], 0.0), axis=1).T
    return dx, route_grad, gate_grad[None], up_grad[None], down_grad[None]


def solution(mesh):
    in_specs = (
        P("ep", None), P("ep", None), P("ep", None), P("ep", None),
        P("ep", "tp", None), P("ep", "tp", None), P("ep", "tp", None),
    )
    out_specs = (
        P("ep", "tp"), P("ep", None), P("ep", "tp", None), P("ep", "tp", None), P("ep", "tp", None),
    )
    return jax.shard_map(
        per_device, mesh=mesh, in_specs=in_specs, out_specs=out_specs, check_vma=False
    )
```

```python
import functools

import jax
import jax.numpy as jnp
from jax import lax
from jax.experimental import pallas as pl
from jax.experimental.pallas import tpu as pltpu
from jax.sharding import PartitionSpec as P

MESH = pl.DeviceIdType.MESH
F32 = jnp.float32
BF16 = jnp.bfloat16


def slices_for(j, tp, bits, count):
    base = j
    for bit in bits:
        base = base - ((j // bit) % 2) * bit
    out = []
    for k in range(count):
        out.append(base + sum(bit for n, bit in enumerate(bits) if (k >> n) & 1))
    return out


def kernel(
    ep, tp, tokens, cotangent, ids, probs, gate_w, up_w, down_w,
    dx_out, route_out, gate_out, up_out, down_out,
    rows, weights, pair_w, wg, part, core_in, tp_in, z_in, grads, totals, r_send, r_in, r_tp,
    load_sem, wz_send, wz_recv, z_send, z_recv, t_send, t_recv, c_send, c_recv,
    pc_send, pc_recv, pt_send, pt_recv, pz_send, pz_recv, rs_send, rs_recv, rt_send, rt_recv, out_sem,
):
    e, j = lax.axis_index("ep"), lax.axis_index("tp")
    levels = ep // 2
    lvl, core = e // 2, e % 2
    t_rows, width = tokens.shape
    span = width // tp
    half = t_rows // 2
    f_rows = gate_w.shape[0]
    nb = tp.bit_length() - 1
    slots = part.shape[0]
    mate = 2 * lvl + 1 - core

    def order(i):
        near = jnp.minimum(lvl, levels - 1 - lvl)
        d = (i + 1) // 2
        close = jnp.where(i % 2 == 1, lvl - d, lvl + d)
        far = jnp.where(lvl == near, lvl + (i - near), lvl - (i - near))
        return jnp.where(i <= 2 * near, close, far)

    def row0(l, c):
        return pl.multiple_of((2 * l + c) * t_rows, t_rows)

    def col(s):
        return pl.ds(pl.multiple_of(s * span, span), span)

    def flip(bit):
        return j + bit * (1 - 2 * ((j // bit) % 2))

    def remote(src, dst, ssem, rsem, de, dt):
        return pltpu.make_async_remote_copy(
            src_ref=src, dst_ref=dst, send_sem=ssem, recv_sem=rsem,
            device_id=(de, dt), device_id_type=MESH)

    own = pl.ds(row0(lvl, core), t_rows)
    loads = [
        pltpu.make_async_copy(tokens, rows.at[0, own], load_sem.at[0]),
        pltpu.make_async_copy(cotangent, rows.at[1, own], load_sem.at[1]),
        pltpu.make_async_copy(gate_w, weights.at[0], load_sem.at[2]),
        pltpu.make_async_copy(up_w, weights.at[1], load_sem.at[3]),
        pltpu.make_async_copy(down_w, weights.at[2], load_sem.at[4]),
    ]
    for copy in loads:
        copy.start()
    barrier = pltpu.get_barrier_semaphore()

    def greet(n, _):
        pl.semaphore_signal(barrier, inc=1, device_id=(lax.rem(e + n, ep), j), device_id_type=MESH)
        return 0

    def greet_tp(n, _):
        pl.semaphore_signal(barrier, inc=1, device_id=(e, lax.rem(j + n, tp)), device_id_type=MESH)
        return 0

    lax.fori_loop(1, ep, greet, 0)
    lax.fori_loop(1, tp, greet_tp, 0)
    pl.semaphore_wait(barrier, ep + tp - 2)

    def w_copy(d):
        return remote(pair_w.at[d], wg.at[e], wz_send.at[d], wz_recv.at[e], d, j)

    def w_wait(src):
        return remote(pair_w.at[src], wg.at[src], wz_send.at[src], wz_recv.at[src], src, j)

    def z_copy(a, l, side):
        ref = rows.at[a, pl.ds(row0(l, core), t_rows), col(j)]
        de = lax.rem(e + (2 if side else ep - 2), ep)
        return remote(ref, ref, z_send.at[a, side, l], z_recv.at[a, l], de, j)

    def gather_step(a, l, s, receive):
        copies = []
        for h in range(2):
            order_bits = [1 << b for b in (range(nb) if h == 0 else range(nb - 1, -1, -1))]
            peer = flip(order_bits[s])
            ids = slices_for(peer if receive else j, tp, order_bits[:s], 1 << s)
            for k, sid in enumerate(ids):
                ref = rows.at[a, pl.ds(row0(l, core) + h * half, half), col(sid)]
                copies.append(remote(
                    ref, ref, t_send.at[a, l, h, (1 << s) - 1 + k], t_recv.at[a, l, h, sid], e, peer))
        return copies

    def core_copy(a, l, c):
        ref = rows.at[a, pl.ds(row0(l, c), t_rows)]
        return remote(ref, ref, c_send.at[a, l], c_recv.at[a, l], mate, j)

    def pc_copy(l, i):
        return remote(part.at[i % slots, 1 - core], core_in.at[l], pc_send.at[l], pc_recv.at[l], mate, j)

    def scatter_step(l, i, s, receive):
        copies = []
        base = sum(tp >> (n + 1) for n in range(s))
        count = tp >> (s + 1)
        for h in range(2):
            order_bits = [1 << b for b in (range(nb) if h == 0 else range(nb - 1, -1, -1))]
            peer = flip(order_bits[s])
            ids = slices_for(j if receive else peer, tp, order_bits[s + 1:], count)
            for k, sid in enumerate(ids):
                src = part.at[i % slots, core, pl.ds(h * half, half), col(sid)]
                dst = tp_in.at[l, h, base + k]
                copies.append((remote(src, dst, pt_send.at[l, h, base + k], pt_recv.at[l, h, base + k], e, peer),
                               src, dst))
        return copies

    def pz_copy(l, i):
        return remote(part.at[i % slots, core, :, col(j)], z_in.at[lvl], pz_send.at[l], pz_recv.at[lvl],
                      2 * l + core, j)

    def pz_wait(src):
        return remote(part.at[0, core, :, col(j)], z_in.at[src], pz_send.at[src], pz_recv.at[src],
                      2 * src + core, j)

    def pair_row(d, _):
        pair_w[d] = jnp.sum(
            jnp.where(ids[...] == d, probs[...].astype(F32), 0.0), axis=0, keepdims=True)
        return 0

    for n in range(2):
        loads[n].wait()
        @pl.when(lvl + 1 < levels)
        def _():
            z_copy(n, lvl, 1).start()
        @pl.when(lvl > 0)
        def _():
            z_copy(n, lvl, 0).start()
        core_copy(n, lvl, core).start()

    lax.fori_loop(0, ep, pair_row, 0)

    def w_start(n, _):
        w_copy(lax.rem(e + n, ep)).start()
        return 0

    lax.fori_loop(1, ep, w_start, 0)
    wg[e] = pair_w[e]
    for n in range(2, 5):
        loads[n].wait()

    def arrive(i):
        l = order(i)
        for a in range(2):
            z_copy(a, l, 0).wait_recv()
            @pl.when(jnp.logical_and(l < lvl, lvl + 1 < levels))
            def _():
                z_copy(a, l, 1).start()
            @pl.when(jnp.logical_and(l > lvl, lvl > 0))
            def _():
                z_copy(a, l, 0).start()
            for copy in gather_step(a, l, 0, False):
                copy.start()

    def spread(i, s):
        l = order(i)
        for a in range(2):
            for copy in gather_step(a, l, s - 1, True):
                copy.wait_recv()
            if s < nb:
                for copy in gather_step(a, l, s, False):
                    copy.start()
            else:
                core_copy(a, l, core).start()

    def compute(i):
        l = order(i)
        for a in range(2):
            core_copy(a, l, 1 - core).wait_recv()
        @pl.when(l != lvl)
        def _():
            w_wait(2 * l).wait_recv()
            w_wait(2 * l + 1).wait_recv()
        @pl.when(l == lvl)
        def _():
            w_wait(mate).wait_recv()
        sel = pl.ds(row0(l, 0), 2 * t_rows)
        nt = (((1,), (1,)), ((), ()))
        x = rows[0, sel, :]
        pre_gate = lax.dot_general(weights[0], x, nt, preferred_element_type=F32)
        pre_up = lax.dot_general(weights[1], x, nt, preferred_element_type=F32)
        back = lax.dot_general(weights[2], rows[1, sel, :], nt, preferred_element_type=F32)
        p = jnp.concatenate([wg[2 * l], wg[2 * l + 1]], axis=1)
        sigma = jax.nn.sigmoid(pre_gate)
        silu = pre_gate * sigma
        hidden = silu * pre_up
        prod = jnp.sum(hidden * back, axis=0, keepdims=True)
        r_send[2 * l] = prod[:, :t_rows]
        r_send[2 * l + 1] = prod[:, t_rows:]
        scaled = p * back
        gg = (scaled * pre_up * sigma * (1.0 + pre_gate * (1.0 - sigma))).astype(BF16)
        gu = (scaled * silu).astype(BF16)
        grads[0, :, sel] = gg
        grads[1, :, sel] = gu
        grads[2, :, sel] = (p * hidden).astype(BF16)
        ggt, gut = gg.T, gu.T
        tile = min(width, 512)

        def column(n, _):
            cs = pl.ds(pl.multiple_of(n * tile, tile), tile)
            d = (jnp.dot(ggt, weights[0, :, cs], preferred_element_type=F32)
                 + jnp.dot(gut, weights[1, :, cs], preferred_element_type=F32)).astype(BF16)
            part[i % slots, 0, :, cs] = d[:t_rows]
            part[i % slots, 1, :, cs] = d[t_rows:]
            return 0

        lax.fori_loop(0, width // tile, column, 0)
        pc_copy(l, i).start()

        def send_r(d):
            remote(r_send.at[d], r_in.at[e], rs_send.at[d], rs_recv.at[e], d, j).start()
        for c in range(2):
            @pl.when(2 * l + c != e)
            def _():
                send_r(2 * l + c)
            @pl.when(2 * l + c == e)
            def _():
                r_in[2 * l + c] = r_send[2 * l + c]

    def merge_core(i):
        l = order(i)
        pc_copy(l, i).wait()
        part[i % slots, core] = (part[i % slots, core].astype(F32) + core_in[l].astype(F32)).astype(BF16)
        for copy, _, _ in scatter_step(l, i, 0, False):
            copy.start()

    def merge_tp(i, s):
        l = order(i)
        for (copy, _, _), (_, mine, got) in zip(scatter_step(l, i, s, False), scatter_step(l, i, s, True)):
            copy.wait()
            mine[...] = (mine[...].astype(F32) + got[...].astype(F32)).astype(BF16)
        if s + 1 < nb:
            for copy, _, _ in scatter_step(l, i, s + 1, False):
                copy.start()
        else:
            @pl.when(l != lvl)
            def _():
                pz_copy(l, i).start()
            @pl.when(l == lvl)
            def _():
                z_in[lvl] = part[i % slots, core, :, col(j)]

    def drain(i):
        l = order(i)
        @pl.when(l != lvl)
        def _():
            pz_copy(l, i).wait_send()

    outs = (gate_out, up_out, down_out)

    def out_copy(k):
        return pltpu.make_async_copy(totals.at[k], outs[k], out_sem.at[k])

    def weight_grad(k):
        tile = min(width, 512)

        def column(n, _):
            cs = pl.ds(pl.multiple_of(n * tile, tile), tile)
            totals[k, :, cs] = jnp.dot(
                grads[k], rows[k // 2, :, cs], preferred_element_type=F32).astype(BF16)
            return 0

        lax.fori_loop(0, width // tile, column, 0)
        out_copy(k).start()

    compute(0)
    d_comp = nb + 1
    last = levels - 1 + d_comp

    def tick(t, _):
        def stage(f, i, low):
            @pl.when(jnp.logical_and(i >= low, i < levels))
            def _():
                f(i)
        def back(late):
            return jnp.where(t == 1 + late, 0, jnp.where(t > d_comp + late, t - d_comp - late, -1))

        for k in range(3):
            @pl.when(t == last + k)
            def _():
                weight_grad(k)
        stage(drain, back(nb + 1), 0)
        for s in range(nb, 0, -1):
            stage(functools.partial(spread, s=s), t - s, 1)
        stage(arrive, t, 1)
        for s in range(nb - 1, -1, -1):
            stage(functools.partial(merge_tp, s=s), back(1 + s), 0)
        stage(compute, t - d_comp + 1, 1)
        stage(merge_core, back(0), 0)
        return 0

    lax.fori_loop(1, levels + d_comp + nb + 1, tick, 0)

    def r_wait(n, _):
        src = lax.rem(e + n, ep)
        remote(r_send.at[src], r_in.at[src], rs_send.at[src], rs_recv.at[src], src, j).wait()
        return 0

    lax.fori_loop(1, ep, r_wait, 0)

    def rt_copy(n):
        dt = lax.rem(j + n, tp)
        return remote(r_in, r_tp.at[j], rt_send.at[dt], rt_recv.at[j], e, dt)

    def rt_wait(n, _):
        src = lax.rem(j + n, tp)
        remote(r_in, r_tp.at[src], rt_send.at[src], rt_recv.at[src], e, src).wait()
        return 0

    def rt_start(n, _):
        rt_copy(n).start()
        return 0

    lax.fori_loop(1, tp, rt_start, 0)
    r_tp[j] = r_in[...]

    def pz_drain(src, _):
        @pl.when(src != lvl)
        def _():
            pz_wait(src).wait_recv()
        return 0

    lax.fori_loop(0, levels, pz_drain, 0)
    dx_out[...] = jnp.sum(z_in[...].astype(F32), axis=0).astype(BF16)
    lax.fori_loop(1, tp, rt_wait, 0)
    r_in[...] = jnp.sum(r_tp[...], axis=0)

    def choose(d, acc):
        return acc + jnp.where(ids[...] == d, r_in[d], 0.0)

    route_out[...] = lax.fori_loop(0, ep, choose, jnp.zeros(route_out.shape, F32))

    for a in range(2):
        @pl.when(lvl + 1 < levels)
        def _():
            z_copy(a, lvl, 1).wait_send()
        @pl.when(lvl > 0)
        def _():
            z_copy(a, lvl, 0).wait_send()

    def finish(l, _):
        for a in range(2):
            core_copy(a, l, core).wait_send()
            @pl.when(jnp.logical_and(l < lvl, lvl + 1 < levels))
            def _():
                z_copy(a, l, 1).wait_send()
            @pl.when(jnp.logical_and(l > lvl, lvl > 0))
            def _():
                z_copy(a, l, 0).wait_send()
            @pl.when(l != lvl)
            def _():
                for s in range(nb):
                    for copy in gather_step(a, l, s, False):
                        copy.wait_send()
        return 0

    lax.fori_loop(0, levels, finish, 0)

    def w_done(n, _):
        w_copy(lax.rem(e + n, ep)).wait_send()
        return 0

    lax.fori_loop(1, ep, w_done, 0)
    for k in range(3):
        out_copy(k).wait()


def per_device(tokens, cotangent, expert_ids, route_weight, gate_weight, up_weight, down_weight):
    ep, tp = lax.axis_size("ep"), lax.axis_size("tp")
    t_rows, width = tokens.shape
    _, f_rows, _ = gate_weight.shape
    levels = ep // 2
    span = width // tp
    slots = min(levels, 8)
    any_, vmem = pl.BlockSpec(memory_space=pl.ANY), pl.BlockSpec(memory_space=pltpu.VMEM)
    dma = pltpu.SemaphoreType.DMA
    big = jax.ShapeDtypeStruct((f_rows, width), BF16)
    scratch = [
        pltpu.VMEM((2, ep * t_rows, width), BF16),
        pltpu.VMEM((3, f_rows, width), BF16),
        pltpu.VMEM((ep, 1, t_rows), F32),
        pltpu.VMEM((ep, 1, t_rows), F32),
        pltpu.VMEM((slots, 2, t_rows, width), BF16),
        pltpu.VMEM((levels, t_rows, width), BF16),
        pltpu.VMEM((levels, 2, tp - 1, t_rows // 2, span), BF16),
        pltpu.VMEM((levels, t_rows, span), BF16),
        pltpu.VMEM((3, f_rows, ep * t_rows), BF16),
        pltpu.VMEM((3, f_rows, width), BF16),
        pltpu.VMEM((ep, 1, t_rows), F32),
        pltpu.VMEM((ep, 1, t_rows), F32),
        pltpu.VMEM((tp, ep, 1, t_rows), F32),
        dma((5,)), dma((ep,)), dma((ep,)), dma((2, 2, levels)), dma((2, levels)),
        dma((2, levels, 2, tp - 1)), dma((2, levels, 2, tp)), dma((2, levels)), dma((2, levels)),
        dma((levels,)), dma((levels,)), dma((levels, 2, tp - 1)), dma((levels, 2, tp - 1)),
        dma((levels,)), dma((levels,)), dma((ep,)), dma((ep,)), dma((tp,)), dma((tp,)), dma((3,)),
    ]
    dx, route, gate_grad, up_grad, down_grad = pl.pallas_call(
        functools.partial(kernel, ep, tp),
        out_shape=(
            jax.ShapeDtypeStruct((t_rows, span), BF16),
            jax.ShapeDtypeStruct(expert_ids.shape[::-1], F32), big, big, big),
        in_specs=[any_, any_, vmem, vmem, any_, any_, any_],
        out_specs=(vmem, vmem, any_, any_, any_),
        scratch_shapes=scratch,
        compiler_params=pltpu.CompilerParams(
            collective_id=0, has_side_effects=True, vmem_limit_bytes=66_000_000),
    )(tokens, cotangent, expert_ids.T, route_weight.T, gate_weight[0], up_weight[0], down_weight[0])
    wide = [g.astype(F32)[None] for g in (gate_grad, up_grad, down_grad)]
    return dx, route.T, *wide


def solution(mesh):
    in_specs = (
        P("ep", None), P("ep", None), P("ep", None), P("ep", None),
        P("ep", "tp", None), P("ep", "tp", None), P("ep", "tp", None),
    )
    out_specs = (
        P("ep", "tp"), P("ep", None), P("ep", "tp", None), P("ep", "tp", None), P("ep", "tp", None),
    )
    return jax.shard_map(
        per_device, mesh=mesh, in_specs=in_specs, out_specs=out_specs, check_vma=False
    )
```
